32 devices in a mesh: fs: 16 (over z, y, x), tp: 2 (over core).
Axes of the slice: x: 2, y: 2, z: 4, core: 2. Of those that a mesh axis runs over, the one named last changes fastest.
Arguments:
- tokens: bfloat16 [5120, 2048], P('fs'), may hold values from -6 to 6
- w_gate: bfloat16 [2048, 5632], P('fs', 'tp'), may hold values from -0.125 to 0.125
- w_up: bfloat16 [2048, 5632], P('fs', 'tp'), may hold values from -0.125 to 0.125
- w_down: bfloat16 [5632, 2048], P('tp', 'fs'), may hold values from -0.078125 to 0.078125
- w_mix_in: bfloat16 [2048, 1024], P('fs', 'tp'), may hold values from -0.125 to 0.125
- w_mix_out: bfloat16 [1024, 2048], P('tp', 'fs'), may hold values from -0.1875 to 0.1875
- pool_w: bfloat16 [8, 128, 128], P('tp'), may hold values from -0.5 to 0.5
- pool_scale: bfloat16 [1024], P('tp'), may hold values from 0.099609375 to 1.8984375
- norm_gains: float32 [6, 2048], replicated, may hold values from 0.1 to 1.9
Outputs:
- layer_out: bfloat16 [5120, 2048], P(('fs', 'tp'))
The draws below stay inside these ranges and needn't reach their ends.
All inputs are finite; a program needn't handle non-finite values.
Results may differ from the reference program's by a relative error of at most 0.018.
Values may be sent and summed in bfloat16 or wider, within the bound.
A program may use at most 128 MiB of HBM per device.

```python
import jax
import jax.numpy as jnp
from jax import lax

D = 2048
FF = 5632
GD = 128
NGROUP = 8
POOLW = 1024
LEN = 64
TOKENS = 5120
N_TP = 2


def levels(stream_key, shape, pieces, least, high):
    level, own = 1.0, jax.random.fold_in(stream_key, 6)
    for axis_at, parts in pieces:
        draws = jnp.exp(jax.random.uniform(jax.random.fold_in(own, axis_at), (parts,), jnp.float32, least / len(pieces), high / len(pieces)))
        level = level * jnp.repeat(draws, shape[axis_at] // parts).reshape([-1 if axis == axis_at else 1 for axis in range(len(shape))])
    return level


def bell_draw(own_key, shape, spread, most, pieces=(), kind=jnp.bfloat16):
    array = jax.random.normal(own_key, shape, jnp.float32) * spread
    if len(pieces) > 0:
        array = levels(own_key, shape, pieces, -0.22, 0.18) * array
    return jnp.clip(array, min=-most, max=most).astype(kind)


def setup_inputs(seed: int = 0) -> dict:
    key_list = jax.random.split(jax.random.key(seed), 10)
    return {
        "tokens": bell_draw(key_list[0], (TOKENS, D), 1.0, 6.0, ((0, 16),)),
        "w_gate": bell_draw(key_list[1], (D, FF), D ** -0.5, 0.125, ((0, 16), (1, 2))),
        "w_up": bell_draw(key_list[2], (D, FF), D ** -0.5, 0.125, ((0, 16), (1, 2))),
        "w_down": bell_draw(key_list[3], (FF, D), FF ** -0.5, 0.078125, ((0, 2), (1, 16))),
        "w_mix_in": bell_draw(key_list[4], (D, POOLW), D ** -0.5, 0.125, ((0, 16), (1, 2))),
        "w_mix_out": bell_draw(key_list[5], (POOLW, D), POOLW ** -0.5, 0.1875, ((0, 2), (1, 16))),
        "pool_w": bell_draw(key_list[6], (NGROUP, GD, GD), GD ** -0.5, 0.5, ((0, 2),)),
        "pool_scale": jnp.clip(1.0 + 0.18 * jax.random.normal(key_list[7], (POOLW,), jnp.float32), 0.099609375, 1.8984375).astype(jnp.bfloat16),
        "norm_gains": jnp.clip(1.0 + 0.18 * jax.random.normal(key_list[8], (6, D), jnp.float32), 0.1, 1.9),
    }


def rms_scale(values, gain):
    return values * lax.rsqrt(lax.optimization_barrier(jnp.mean(values * values, axis=-1, keepdims=True)) + 1e-06) * gain

def split_sum(left_rows, right_matrix):
    block_width = left_rows.shape[1] // N_TP

    def add_block(block_id, running_sum):
        offset = (block_id * block_width).astype(jnp.int32)
        left_part = lax.dynamic_slice_in_dim(left_rows, offset, block_width, 1)
        right_part = lax.dynamic_slice_in_dim(right_matrix, offset, block_width, 0)
        partial_value = jnp.dot(left_part, right_part, preferred_element_type=jnp.float32).astype(jnp.bfloat16)
        partial_value = lax.optimization_barrier(partial_value)
        return running_sum + partial_value.astype(jnp.float32)
    initial = jnp.zeros((left_rows.shape[0], right_matrix.shape[1]), jnp.float32)
    return lax.fori_loop(0, N_TP, add_block, initial)

def gated(normed, w_gate, w_up):
    gate_part = jnp.dot(normed, w_gate, preferred_element_type=jnp.float32)
    up_part = jnp.dot(normed, w_up, preferred_element_type=jnp.float32)
    return (jax.nn.silu(gate_part) * up_part).astype(jnp.bfloat16)

def pool_mix(pooled_in, pool_w, pool_scale):
    values = pooled_in.astype(jnp.float32).reshape(-1, LEN, NGROUP, GD)
    totals = jnp.cumsum(values, axis=1)
    position = jnp.arange(1, LEN + 1).astype(jnp.float32)[None, :, None]
    averages = []
    for group_id in range(NGROUP):
        window = 2 ** (1 + group_id % 4)
        running = totals[:, :, group_id]
        lagged = jnp.pad(running, ((0, 0), (window, 0), (0, 0)))[:, :LEN]
        averages.append((running - lagged) / jnp.minimum(position, float(window)))
    average = jnp.stack(averages, axis=2)
    deviation = (average - values).astype(jnp.bfloat16)
    regrouped = jnp.einsum('btgi,gio->btgo', deviation.astype(jnp.float32), pool_w.astype(jnp.float32))
    regrouped = regrouped.reshape(-1, NGROUP * GD) * pool_scale.astype(jnp.float32)
    return regrouped.astype(jnp.bfloat16)

def reference(tokens, w_gate, w_up, w_down, w_mix_in, w_mix_out, pool_w, pool_scale, norm_gains):
    scales = norm_gains.astype(jnp.float32)
    stream = tokens.astype(jnp.float32)
    normed = rms_scale(stream, scales[0]).astype(jnp.bfloat16)
    stream = stream + 0.5 * rms_scale(split_sum(gated(normed, w_gate, w_up), w_down), scales[1])
    normed = rms_scale(stream, scales[2]).astype(jnp.bfloat16)
    pooled_in = jnp.dot(normed, w_mix_in, preferred_element_type=jnp.float32).astype(jnp.bfloat16)
    stream = stream + rms_scale(split_sum(pool_mix(pooled_in, pool_w, pool_scale), w_mix_out), scales[3])
    normed = rms_scale(stream, scales[4]).astype(jnp.bfloat16)
    stream = stream + 0.5 * rms_scale(split_sum(gated(normed, w_gate, w_up), w_down), scales[5])
    return stream.astype(jnp.bfloat16)
```

```python
import functools
import itertools

import jax
import jax.numpy as jnp
from jax import lax
from jax.experimental import pallas as pl
from jax.experimental.pallas import tpu as pltpu
from jax.sharding import PartitionSpec as P

LEN = 64
MESH = pl.DeviceIdType.MESH


def line_dims(mesh):
    devices = mesh.devices.reshape(mesh.shape["fs"], -1)[:, 0]
    count = len(devices)
    coords = [tuple(getattr(d, "coords", ())) for d in devices]
    dims = []
    for axis in range(len(coords[0])):
        values = sorted({c[axis] for c in coords})
        if len(values) > 1:
            stride = next(i for i in range(count) if coords[i][axis] != coords[0][axis])
            dims.append((len(values), stride, axis, values))
    dims.sort(key=lambda d: -d[1])
    good = len(dims) > 0 and all(
        sum(vals.index(c[axis]) * stride for _, stride, axis, vals in dims) == i
        for i, c in enumerate(coords)
    )
    if not good:
        return ((count, 1),)
    return tuple((d[0], d[1]) for d in dims)


def near(position, size, rank):
    inner = jnp.minimum(position, size - 1 - position)
    alternating = rank <= 2 * inner
    distance = jnp.where(alternating, (rank + 1) // 2, rank - inner)
    toward_high = jnp.where(alternating, rank % 2 == 1, 2 * position < size - 1)
    step = jnp.where(toward_high, 1, -1)
    return position + step * distance, -step


def piece_plan(dims, order):
    sizes = [dims[d][0] for d in order]
    slots = []
    for ranks in itertools.product(*[range(n) for n in sizes]):
        slots.append(ranks)
    slots.sort(key=lambda r: (sum(r), r))
    return slots


class Piece:
    def __init__(self, index, dims, order, src_of, dst_of):
        self.index, self.dims, self.order = index, dims, order
        self.src_of, self.dst_of = src_of, dst_of
        self.slots = piece_plan(dims, order)

    def locate(self, me, ranks):
        source, last, away = me, -1, None
        for place, (d, rank) in enumerate(zip(self.order, ranks)):
            if rank > 0:
                size, stride = self.dims[d]
                position = (me // stride) % size
                found, step = near(position, size, rank)
                source = source + (found - position) * stride
                last, away = place, step
        return source, last, away

    def sends(self, me, ranks):
        _, last, away = self.locate(me, ranks)
        out = []
        for place, d in enumerate(self.order):
            size, stride = self.dims[d]
            position = (me // stride) % size
            if place == last:
                if size > 2:
                    ok = jnp.logical_and(position + away >= 0, position + away < size)
                    out.append((ok, me + away * stride))
            elif place > last:
                if size == 2:
                    out.append((None, me + (1 - 2 * position) * stride))
                else:
                    out.append((position + 1 < size, me + stride))
                    out.append((position > 0, me - stride))
        return out


def when(condition, act):
    if condition is None:
        act()
    else:
        pl.when(condition)(act)


def spread(pieces, me, chunk, send_sem, recv_sem, low, high, mode):
    todo = []
    for piece in pieces:
        for ranks in piece.slots:
            todo.append((sum(ranks), piece, ranks))
    todo.sort(key=lambda t: t[0])
    for depth, piece, ranks in todo:
        if not low <= depth < high:
            continue
        source, last, _ = piece.locate(me, ranks)
        landed = piece.dst_of(chunk, source)
        origin = piece.src_of(chunk) if depth == 0 else landed
        recv = recv_sem.at[chunk, piece.index, source]
        if depth > 0 and mode == "start":
            pltpu.make_async_copy(landed, landed, recv).wait()
        base = piece.first_send[ranks]
        for offset, (ok, target) in enumerate(piece.sends(me, ranks)):
            copy = pltpu.make_async_remote_copy(
                src_ref=origin,
                dst_ref=landed,
                send_sem=send_sem.at[chunk, base + offset],
                recv_sem=recv,
                device_id={"fs": target},
                device_id_type=MESH,
            )
            when(ok, copy.start if mode == "start" else copy.wait_send)


def number_sends(pieces):
    total = 0
    for piece in pieces:
        piece.first_send = {}
        for ranks in piece.slots:
            piece.first_send[ranks] = total
            last = max([i for i, r in enumerate(ranks) if r > 0], default=-1)
            for place, d in enumerate(piece.order):
                size = piece.dims[d][0]
                if place == last:
                    total += 1 if size > 2 else 0
                elif place > last:
                    total += 1 if size == 2 else 2
    return total


def cut(extent, unit, share):
    return max(unit, min(extent - unit, round(extent * share / unit) * unit))


def gather_plan(dims, refs, outs, block, blocks):
    gate, up, down, mix_in, mix_out = refs
    gate_o, up_o, down_o, mix_in_o, mix_out_o = outs
    n = len(dims)
    first = tuple(range(n))
    second = first[1:] + first[:1]
    third = first[-1:] + first[:-1]
    depth, width = gate.shape
    across = down.shape[1]
    mixed = mix_in.shape[1]
    pooled = mix_out.shape[0]

    def columns(ref, out, start_of, size):
        return (
            lambda c: ref.at[:, pl.ds(start_of(c), size)],
            lambda c, s: out.at[pl.ds(s * depth, depth), pl.ds(start_of(c), size)],
        )

    def rows(ref, out, start_of, size):
        def dst(c, s):
            if len(out.shape) == 3:
                return out.at[s, pl.ds(start_of(c), size), :]
            return out.at[pl.ds(start_of(c), size), pl.ds(s * across, across)]

        return (lambda c: ref.at[pl.ds(start_of(c), size), :], dst)

    def at(offset):
        if blocks == 1:
            return lambda c: offset
        return lambda c: pl.multiple_of(c * block + offset, 16 if offset else block)

    down_cut = cut(block, 16, 2 / 3)
    main = [
        Piece(0, dims, first, *columns(gate, gate_o, at(0), block)),
        Piece(1, dims, third, *columns(up, up_o, at(0), block)),
        Piece(2, dims, first, *rows(down, down_o, at(0), down_cut)),
        Piece(3, dims, second, *rows(down, down_o, at(down_cut), block - down_cut)),
    ]
    mix_cut = cut(pooled, 16, 2 / 3)

    def fixed(offset):
        return lambda c: offset

    mix = [
        Piece(0, dims, first, *columns(mix_in, mix_in_o, fixed(0), mixed)),
        Piece(1, dims, third, *rows(mix_out, mix_out_o, fixed(0), mix_cut)),
        Piece(2, dims, second, *rows(mix_out, mix_out_o, fixed(mix_cut), pooled - mix_cut)),
    ]
    return main, mix


def gather_kernel(dims, block, blocks, *args):
    refs, outs = args[:5], args[5:10]
    send_sem, recv_sem, local_sem = args[10:]
    me = lax.axis_index("fs")
    barrier = pltpu.get_barrier_semaphore()
    expected = 0
    for size, stride in dims:
        position = (me // stride) % size
        for step, ok in ((1, position + 1 < size), (-1, position > 0)):
            def signal(step=step, stride=stride):
                pl.semaphore_signal(
                    barrier, inc=1, device_id={"fs": me + step * stride}, device_id_type=MESH
                )

            pl.when(ok)(signal)
            expected = expected + jnp.where(ok, 1, 0)
    pl.semaphore_wait(barrier, expected)

    main, mix = gather_plan(dims, refs, outs, block, blocks)
    number_sends(main)
    number_sends(mix)
    deepest = sum(size - 1 for size, _ in dims) + 1
    early = min(3, deepest)

    locals_ = []
    for i, (ref, out) in enumerate(zip(refs, outs)):
        rows_here, columns_here = ref.shape
        if len(out.shape) == 3:
            target = out.at[me]
        elif i in (0, 1, 3):
            target = out.at[pl.ds(me * rows_here, rows_here), :]
        else:
            target = out.at[:, pl.ds(me * columns_here, columns_here)]
        locals_.append(pltpu.make_async_copy(ref, target, local_sem.at[i]))

    go = functools.partial(spread, send_sem=send_sem, recv_sem=recv_sem)
    go(main, me, 0, low=0, high=1, mode="start")
    for copy in locals_:
        copy.start()

    def step(i, carry):
        @pl.when(i + 1 < blocks)
        def _():
            go(main, me, i + 1, low=0, high=1, mode="start")

        go(main, me, i, low=1, high=early, mode="start")

        @pl.when(i > 0)
        def _():
            go(main, me, i - 1, low=early, high=deepest, mode="start")

        return carry

    lax.fori_loop(0, blocks, step, 0)
    go(mix, me, blocks, low=0, high=1, mode="start")
    go(main, me, blocks - 1, low=early, high=deepest, mode="start")
    go(mix, me, blocks, low=1, high=deepest, mode="start")

    def finish(i, carry):
        go(main, me, i, low=0, high=deepest, mode="end")
        return carry

    lax.fori_loop(0, blocks, finish, 0)
    go(mix, me, blocks, low=0, high=deepest, mode="end")
    for copy in locals_:
        copy.wait()


def gather_weights(dims, w_gate, w_up, w_down, w_mix_in, w_mix_out):
    count = 1
    for size, _ in dims:
        count *= size
    width = w_gate.shape[1]
    block = next((b for b in (256, 128) if width % b == 0), width)
    blocks = width // block

    def rows_out(a):
        return jax.ShapeDtypeStruct((a.shape[0] * count, a.shape[1]), a.dtype)

    def columns_out(a):
        if a.shape[1] % 128 == 0:
            return jax.ShapeDtypeStruct((a.shape[0], a.shape[1] * count), a.dtype)
        return jax.ShapeDtypeStruct((count, *a.shape), a.dtype)

    shapes = [rows_out(w_gate), rows_out(w_up), columns_out(w_down)]
    shapes += [rows_out(w_mix_in), columns_out(w_mix_out)]
    class Shape:
        def __init__(self, shape):
            self.shape = shape

    stand_in = [Shape(a.shape) for a in (w_gate, w_up, w_down, w_mix_in, w_mix_out)]
    main, mix = gather_plan(dims, stand_in, [Shape(s.shape) for s in shapes], block, blocks)
    sends = max(number_sends(main), number_sends(mix))
    outs = pl.pallas_call(
        functools.partial(gather_kernel, dims, block, blocks),
        out_shape=shapes,
        in_specs=[pl.BlockSpec(memory_space=pltpu.HBM)] * 5,
        out_specs=[pl.BlockSpec(memory_space=pltpu.HBM)] * 5,
        scratch_shapes=[
            pltpu.SemaphoreType.DMA((blocks + 1, sends)),
            pltpu.SemaphoreType.DMA((blocks + 1, len(main), count)),
            pltpu.SemaphoreType.DMA((5,)),
        ],
        compiler_params=pltpu.CompilerParams(collective_id=0, has_side_effects=True),
        name="gather_weights",
    )(w_gate, w_up, w_down, w_mix_in, w_mix_out)

    def flat(a):
        if a.ndim == 2:
            return a
        return jnp.transpose(a, (1, 0, 2)).reshape(a.shape[1], -1)

    return [flat(a) for a in outs]


def rms_scale(values, gain):
    return values * lax.rsqrt(jnp.mean(values * values, axis=-1, keepdims=True) + 1e-06) * gain


def reduce_rows(left_rows, right_matrix):
    return lax.psum_scatter(
        jnp.dot(left_rows, right_matrix, preferred_element_type=jnp.float32).astype(jnp.bfloat16),
        "tp",
        scatter_dimension=0,
        tiled=True,
    ).astype(jnp.float32)


def gather_rows(normed, project):
    return project(lax.all_gather(normed, "tp", axis=0, tiled=True), jnp.int32(0))


def body(dims, tokens, w_gate, w_up, w_down, w_mix_in, w_mix_out, pool_w, pool_scale, norm_gains):
    tp_size = lax.axis_size("tp")
    rows_all = tokens.shape[0]
    own_rows = rows_all // tp_size
    stream = tokens.astype(jnp.float32)
    normed = rms_scale(stream, norm_gains[0]).astype(jnp.bfloat16)
    gate_full, up_full, down_full, mix_in_full, mix_out_full = gather_weights(
        dims, w_gate, w_up, w_down, w_mix_in, w_mix_out
    )
    gate_first = jnp.dot(normed, gate_full, preferred_element_type=jnp.float32)
    up_first = jnp.dot(normed, up_full, preferred_element_type=jnp.float32)
    hidden = (jax.nn.silu(gate_first) * up_first).astype(jnp.bfloat16)
    stream_own = lax.dynamic_slice_in_dim(stream, lax.axis_index("tp") * own_rows, own_rows, 0)
    stream_own = stream_own + 0.5 * rms_scale(reduce_rows(hidden, down_full), norm_gains[1])
    normed = rms_scale(stream_own, norm_gains[2]).astype(jnp.bfloat16)

    def project_pool(part_rows, offset):
        return jnp.dot(part_rows, mix_in_full, preferred_element_type=jnp.float32).astype(
            jnp.bfloat16
        )

    pooled_in = gather_rows(normed, project_pool)
    groups_here = pool_w.shape[0]
    group_dim = pool_w.shape[1]
    values = pooled_in.astype(jnp.float32).reshape(rows_all // LEN, LEN, groups_here, group_dim)
    totals = jnp.cumsum(values, axis=1)
    position = jnp.arange(1, LEN + 1).astype(jnp.float32)[None, :, None, None]
    window_ids = (lax.axis_index("tp") * groups_here + jnp.arange(groups_here)) % 4
    average = jnp.zeros_like(values)
    for window_slot in range(4):
        window = 2 ** (1 + window_slot)
        lagged = jnp.pad(totals, ((0, 0), (window, 0), (0, 0), (0, 0)))[:, :LEN]
        candidate = (totals - lagged) / jnp.minimum(position, float(window))
        average = jnp.where((window_ids == window_slot)[None, None, :, None], candidate, average)
    deviation = (average - values).astype(jnp.bfloat16)
    regrouped = jnp.einsum("btgi,gio->btgo", deviation, pool_w, preferred_element_type=jnp.float32)
    regrouped = (
        regrouped.reshape(rows_all, groups_here * group_dim) * pool_scale.astype(jnp.float32)
    ).astype(jnp.bfloat16)
    stream_own = stream_own + rms_scale(reduce_rows(regrouped, mix_out_full), norm_gains[3])
    normed = rms_scale(stream_own, norm_gains[4]).astype(jnp.bfloat16)

    def project_ffn(part_rows, offset):
        gate_part = jnp.dot(part_rows, gate_full, preferred_element_type=jnp.float32)
        up_part = jnp.dot(part_rows, up_full, preferred_element_type=jnp.float32)
        return (jax.nn.silu(gate_part) * up_part).astype(jnp.bfloat16)

    hidden = gather_rows(normed, project_ffn)
    stream_own = stream_own + 0.5 * rms_scale(reduce_rows(hidden, down_full), norm_gains[5])
    return stream_own.astype(jnp.bfloat16)


def solution(mesh):
    in_specs = (
        P("fs", None),
        P("fs", "tp"),
        P("fs", "tp"),
        P("tp", "fs"),
        P("fs", "tp"),
        P("tp", "fs"),
        P("tp", None, None),
        P("tp"),
        P(),
    )
    out_specs = P(("fs", "tp"), None)
    return jax.shard_map(functools.partial(body, line_dims(mesh)), mesh=mesh, in_specs=in_specs, out_specs=out_specs, check_vma=False)
```

```python
import functools
import itertools

import jax
import jax.numpy as jnp
from jax import lax
from jax.experimental import pallas as pl
from jax.experimental.pallas import tpu as pltpu
from jax.sharding import PartitionSpec as P

LEN = 64
MESH = pl.DeviceIdType.MESH


def line_dims(mesh):
    devices = mesh.devices.reshape(mesh.shape["fs"], -1)[:, 0]
    count = len(devices)
    coords = [tuple(getattr(d, "coords", ())) for d in devices]
    dims = []
    for axis in range(len(coords[0])):
        values = sorted({c[axis] for c in coords})
        if len(values) > 1:
            stride = next(i for i in range(count) if coords[i][axis] != coords[0][axis])
            dims.append((len(values), stride, axis, values))
    dims.sort(key=lambda d: -d[1])
    good = len(dims) > 0 and all(
        sum(vals.index(c[axis]) * stride for _, stride, axis, vals in dims) == i
        for i, c in enumerate(coords)
    )
    if not good:
        return ((count, 1),)
    return tuple((d[0], d[1]) for d in dims)


def near(position, size, rank):
    inner = jnp.minimum(position, size - 1 - position)
    alternating = rank <= 2 * inner
    distance = jnp.where(alternating, (rank + 1) // 2, rank - inner)
    toward_high = jnp.where(alternating, rank % 2 == 1, 2 * position < size - 1)
    step = jnp.where(toward_high, 1, -1)
    return position + step * distance, -step


def piece_plan(dims, order):
    sizes = [dims[d][0] for d in order]
    slots = []
    for ranks in itertools.product(*[range(n) for n in sizes]):
        slots.append(ranks)
    slots.sort(key=lambda r: (sum(r), r))
    return slots


class Piece:
    def __init__(self, index, dims, order, src_of, dst_of):
        self.index, self.dims, self.order = index, dims, order
        self.src_of, self.dst_of = src_of, dst_of
        self.slots = piece_plan(dims, order)

    def locate(self, me, ranks):
        source, last, away = me, -1, None
        for place, (d, rank) in enumerate(zip(self.order, ranks)):
            if rank > 0:
                size, stride = self.dims[d]
                position = (me // stride) % size
                found, step = near(position, size, rank)
                source = source + (found - position) * stride
                last, away = place, step
        return source, last, away

    def sends(self, me, ranks):
        _, last, away = self.locate(me, ranks)
        out = []
        for place, d in enumerate(self.order):
            size, stride = self.dims[d]
            position = (me // stride) % size
            if place == last:
                if size > 2:
                    ok = jnp.logical_and(position + away >= 0, position + away < size)
                    out.append((ok, me + away * stride))
            elif place > last:
                if size == 2:
                    out.append((None, me + (1 - 2 * position) * stride))
                else:
                    out.append((position + 1 < size, me + stride))
                    out.append((position > 0, me - stride))
        return out


def when(condition, act):
    if condition is None:
        act()
    else:
        pl.when(condition)(act)


def spread(pieces, me, chunk, send_sem, recv_sem, low, high, mode):
    todo = []
    for piece in pieces:
        for ranks in piece.slots:
            todo.append((sum(ranks), piece, ranks))
    todo.sort(key=lambda t: t[0])
    for depth, piece, ranks in todo:
        if not low <= depth < high:
            continue
        source, last, _ = piece.locate(me, ranks)
        landed = piece.dst_of(chunk, source)
        origin = piece.src_of(chunk) if depth == 0 else landed
        recv = recv_sem.at[chunk, piece.index, source]
        if depth > 0 and mode == "start":
            pltpu.make_async_copy(landed, landed, recv).wait()
        base = piece.first_send[ranks]
        for offset, (ok, target) in enumerate(piece.sends(me, ranks)):
            copy = pltpu.make_async_remote_copy(
                src_ref=origin,
                dst_ref=landed,
                send_sem=send_sem.at[chunk, base + offset],
                recv_sem=recv,
                device_id={"fs": target},
                device_id_type=MESH,
            )
            when(ok, copy.start if mode == "start" else copy.wait_send)


def number_sends(pieces):
    total = 0
    for piece in pieces:
        piece.first_send = {}
        for ranks in piece.slots:
            piece.first_send[ranks] = total
            last = max([i for i, r in enumerate(ranks) if r > 0], default=-1)
            for place, d in enumerate(piece.order):
                size = piece.dims[d][0]
                if place == last:
                    total += 1 if size > 2 else 0
                elif place > last:
                    total += 1 if size == 2 else 2
    return total


def cut(extent, unit, share):
    return max(unit, min(extent - unit, round(extent * share / unit) * unit))


def gather_plan(dims, refs, outs, block, blocks):
    gate, up, down, mix_in, mix_out = refs
    gate_o, up_o, down_o, mix_in_o, mix_out_o = outs
    n = len(dims)
    first = tuple(range(n))
    second = first[1:] + first[:1]
    third = first[-1:] + first[:-1]
    depth, width = gate.shape
    across = down.shape[1]
    mixed = mix_in.shape[1]
    pooled = mix_out.shape[0]

    def columns(ref, out, start_of, size):
        return (
            lambda c: ref.at[:, pl.ds(start_of(c), size)],
            lambda c, s: out.at[pl.ds(s * depth, depth), pl.ds(start_of(c), size)],
        )

    def rows(ref, out, start_of, size):
        def dst(c, s):
            if len(out.shape) == 3:
                return out.at[s, pl.ds(start_of(c), size), :]
            return out.at[pl.ds(start_of(c), size), pl.ds(s * across, across)]

        return (lambda c: ref.at[pl.ds(start_of(c), size), :], dst)

    def at(offset):
        if blocks == 1:
            return lambda c: offset
        return lambda c: pl.multiple_of(c * block + offset, 16 if offset else block)

    down_cut = cut(block, 16, 2 / 3)
    main = [
        Piece(0, dims, first, *columns(gate, gate_o, at(0), block)),
        Piece(1, dims, third, *columns(up, up_o, at(0), block)),
        Piece(2, dims, first, *rows(down, down_o, at(0), down_cut)),
        Piece(3, dims, second, *rows(down, down_o, at(down_cut), block - down_cut)),
    ]
    mix_cut = cut(pooled, 16, 2 / 3)

    def fixed(offset):
        return lambda c: offset

    mix = [
        Piece(0, dims, first, *columns(mix_in, mix_in_o, fixed(0), mixed)),
        Piece(1, dims, third, *rows(mix_out, mix_out_o, fixed(0), mix_cut)),
        Piece(2, dims, second, *rows(mix_out, mix_out_o, fixed(mix_cut), pooled - mix_cut)),
    ]
    return main, mix


def gather_kernel(dims, block, blocks, *args):
    refs, outs = args[:5], args[5:10]
    send_sem, recv_sem, local_sem = args[10:]
    me = lax.axis_index("fs")
    barrier = pltpu.get_barrier_semaphore()
    expected = 0
    for size, stride in dims:
        position = (me // stride) % size
        for step, ok in ((1, position + 1 < size), (-1, position > 0)):
            def signal(step=step, stride=stride):
                pl.semaphore_signal(
                    barrier, inc=1, device_id={"fs": me + step * stride}, device_id_type=MESH
                )

            pl.when(ok)(signal)
            expected = expected + jnp.where(ok, 1, 0)
    pl.semaphore_wait(barrier, expected)

    main, mix = gather_plan(dims, refs, outs, block, blocks)
    number_sends(main)
    number_sends(mix)
    deepest = sum(size - 1 for size, _ in dims) + 1
    early = min(3, deepest)

    locals_ = []
    for i, (ref, out) in enumerate(zip(refs, outs)):
        rows_here, columns_here = ref.shape
        if len(out.shape) == 3:
            target = out.at[me]
        elif i in (0, 1, 3):
            target = out.at[pl.ds(me * rows_here, rows_here), :]
        else:
            target = out.at[:, pl.ds(me * columns_here, columns_here)]
        locals_.append(pltpu.make_async_copy(ref, target, local_sem.at[i]))

    go = functools.partial(spread, send_sem=send_sem, recv_sem=recv_sem)
    go(main, me, 0, low=0, high=1, mode="start")
    for copy in locals_:
        copy.start()

    def step(i, carry):
        @pl.when(i + 1 < blocks)
        def _():
            go(main, me, i + 1, low=0, high=1, mode="start")

        go(main, me, i, low=1, high=early, mode="start")

        @pl.when(i > 0)
        def _():
            go(main, me, i - 1, low=early, high=deepest, mode="start")

        return carry

    lax.fori_loop(0, blocks, step, 0)
    go(mix, me, blocks, low=0, high=1, mode="start")
    go(main, me, blocks - 1, low=early, high=deepest, mode="start")
    go(mix, me, blocks, low=1, high=deepest, mode="start")

    def finish(i, carry):
        go(main, me, i, low=0, high=deepest, mode="end")
        return carry

    lax.fori_loop(0, blocks, finish, 0)
    go(mix, me, blocks, low=0, high=deepest, mode="end")
    for copy in locals_:
        copy.wait()


def gather_weights(dims, w_gate, w_up, w_down, w_mix_in, w_mix_out):
    count = 1
    for size, _ in dims:
        count *= size
    width = w_gate.shape[1]
    block = next((b for b in (256, 128) if width % b == 0), width)
    blocks = width // block

    def rows_out(a):
        return jax.ShapeDtypeStruct((a.shape[0] * count, a.shape[1]), a.dtype)

    def columns_out(a):
        if a.shape[1] % 128 == 0:
            return jax.ShapeDtypeStruct((a.shape[0], a.shape[1] * count), a.dtype)
        return jax.ShapeDtypeStruct((count, *a.shape), a.dtype)

    shapes = [rows_out(w_gate), rows_out(w_up), columns_out(w_down)]
    shapes += [rows_out(w_mix_in), columns_out(w_mix_out)]
    class Shape:
        def __init__(self, shape):
            self.shape = shape

    stand_in = [Shape(a.shape) for a in (w_gate, w_up, w_down, w_mix_in, w_mix_out)]
    main, mix = gather_plan(dims, stand_in, [Shape(s.shape) for s in shapes], block, blocks)
    sends = max(number_sends(main), number_sends(mix))
    outs = pl.pallas_call(
        functools.partial(gather_kernel, dims, block, blocks),
        out_shape=shapes,
        in_specs=[pl.BlockSpec(memory_space=pltpu.HBM)] * 5,
        out_specs=[pl.BlockSpec(memory_space=pltpu.HBM)] * 5,
        scratch_shapes=[
            pltpu.SemaphoreType.DMA((blocks + 1, sends)),
            pltpu.SemaphoreType.DMA((blocks + 1, len(main), count)),
            pltpu.SemaphoreType.DMA((5,)),
        ],
        compiler_params=pltpu.CompilerParams(collective_id=0, has_side_effects=True),
        name="gather_weights",
    )(w_gate, w_up, w_down, w_mix_in, w_mix_out)

    def flat(a):
        if a.ndim == 2:
            return a
        return jnp.transpose(a, (1, 0, 2)).reshape(a.shape[1], -1)

    return [flat(a) for a in outs]


def rms_scale(values, gain):
    return values * lax.rsqrt(jnp.mean(values * values, axis=-1, keepdims=True) + 1e-06) * gain


def total_over_tp(left_rows, right_matrix):
    part = jnp.dot(left_rows, right_matrix, preferred_element_type=jnp.float32)
    part = part.astype(jnp.bfloat16)
    if lax.axis_size("tp") == 2:
        other = lax.ppermute(part, "tp", ((0, 1), (1, 0)))
        return part.astype(jnp.float32) + other.astype(jnp.float32)
    return lax.psum(part.astype(jnp.float32), "tp")


def own_total_over_tp(left_rows, right_matrix):
    part = jnp.dot(left_rows, right_matrix, preferred_element_type=jnp.float32)
    part = part.astype(jnp.bfloat16)
    if lax.axis_size("tp") == 2:
        mine = own_rows_of(part)
        half = mine.shape[0]
        theirs = lax.dynamic_slice_in_dim(part, (1 - lax.axis_index("tp")) * half, half, 0)
        other = lax.ppermute(theirs, "tp", ((0, 1), (1, 0)))
        return mine.astype(jnp.float32) + other.astype(jnp.float32)
    return lax.psum_scatter(part.astype(jnp.float32), "tp", scatter_dimension=0, tiled=True)


def own_rows_of(array):
    count = array.shape[0] // lax.axis_size("tp")
    return lax.dynamic_slice_in_dim(array, lax.axis_index("tp") * count, count, 0)


def body(dims, tokens, w_gate, w_up, w_down, w_mix_in, w_mix_out, pool_w, pool_scale, norm_gains):
    rows_all = tokens.shape[0]
    stream = tokens.astype(jnp.float32)
    normed = rms_scale(stream, norm_gains[0]).astype(jnp.bfloat16)
    gate_full, up_full, down_full, mix_in_full, mix_out_full = gather_weights(
        dims, w_gate, w_up, w_down, w_mix_in, w_mix_out
    )
    gate_first = jnp.dot(normed, gate_full, preferred_element_type=jnp.float32)
    up_first = jnp.dot(normed, up_full, preferred_element_type=jnp.float32)
    hidden = (jax.nn.silu(gate_first) * up_first).astype(jnp.bfloat16)
    stream = stream + 0.5 * rms_scale(total_over_tp(hidden, down_full), norm_gains[1])
    normed = rms_scale(stream, norm_gains[2]).astype(jnp.bfloat16)
    pooled_in = jnp.dot(normed, mix_in_full, preferred_element_type=jnp.float32)
    pooled_in = pooled_in.astype(jnp.bfloat16)
    groups_here = pool_w.shape[0]
    group_dim = pool_w.shape[1]
    values = pooled_in.astype(jnp.float32).reshape(rows_all // LEN, LEN, groups_here, group_dim)
    totals = jnp.cumsum(values, axis=1)
    position = jnp.arange(1, LEN + 1).astype(jnp.float32)[None, :, None, None]
    window_ids = (lax.axis_index("tp") * groups_here + jnp.arange(groups_here)) % 4
    average = jnp.zeros_like(values)
    for window_slot in range(4):
        window = 2 ** (1 + window_slot)
        lagged = jnp.pad(totals, ((0, 0), (window, 0), (0, 0), (0, 0)))[:, :LEN]
        candidate = (totals - lagged) / jnp.minimum(position, float(window))
        average = jnp.where((window_ids == window_slot)[None, None, :, None], candidate, average)
    deviation = (average - values).astype(jnp.bfloat16)
    regrouped = jnp.einsum("btgi,gio->btgo", deviation, pool_w, preferred_element_type=jnp.float32)
    regrouped = (
        regrouped.reshape(rows_all, groups_here * group_dim) * pool_scale.astype(jnp.float32)
    ).astype(jnp.bfloat16)
    stream = stream + rms_scale(total_over_tp(regrouped, mix_out_full), norm_gains[3])
    normed = rms_scale(stream, norm_gains[4]).astype(jnp.bfloat16)
    gate_second = jnp.dot(normed, gate_full, preferred_element_type=jnp.float32)
    up_second = jnp.dot(normed, up_full, preferred_element_type=jnp.float32)
    hidden = (jax.nn.silu(gate_second) * up_second).astype(jnp.bfloat16)
    stream_own = own_rows_of(stream)
    stream_own = stream_own + 0.5 * rms_scale(own_total_over_tp(hidden, down_full), norm_gains[5])
    return stream_own.astype(jnp.bfloat16)


def solution(mesh):
    in_specs = (
        P("fs", None),
        P("fs", "tp"),
        P("fs", "tp"),
        P("tp", "fs"),
        P("fs", "tp"),
        P("tp", "fs"),
        P("tp", None, None),
        P("tp"),
        P(),
    )
    out_specs = P(("fs", "tp"), None)
    return jax.shard_map(functools.partial(body, line_dims(mesh)), mesh=mesh, in_specs=in_specs, out_specs=out_specs, check_vma=False)
```

```python
import functools
import itertools

import jax
import jax.numpy as jnp
from jax import lax
from jax.experimental import pallas as pl
from jax.experimental.pallas import tpu as pltpu
from jax.sharding import PartitionSpec as P

LEN = 64
MESH = pl.DeviceIdType.MESH


def line_dims(mesh):
    devices = mesh.devices.reshape(mesh.shape["fs"], -1)[:, 0]
    count = len(devices)
    coords = [tuple(getattr(d, "coords", ())) for d in devices]
    dims = []
    for axis in range(len(coords[0])):
        values = sorted({c[axis] for c in coords})
        if len(values) > 1:
            stride = next(i for i in range(count) if coords[i][axis] != coords[0][axis])
            dims.append((len(values), stride, axis, values))
    dims.sort(key=lambda d: -d[1])
    good = len(dims) > 0 and all(
        sum(vals.index(c[axis]) * stride for _, stride, axis, vals in dims) == i
        for i, c in enumerate(coords)
    )
    if not good:
        return ((count, 1),)
    return tuple((d[0], d[1]) for d in dims)


def near(position, size, rank):
    inner = jnp.minimum(position, size - 1 - position)
    alternating = rank <= 2 * inner
    distance = jnp.where(alternating, (rank + 1) // 2, rank - inner)
    toward_high = jnp.where(alternating, rank % 2 == 1, 2 * position < size - 1)
    step = jnp.where(toward_high, 1, -1)
    return position + step * distance, -step


def piece_plan(dims, order):
    sizes = [dims[d][0] for d in order]
    slots = []
    for ranks in itertools.product(*[range(n) for n in sizes]):
        slots.append(ranks)
    slots.sort(key=lambda r: (sum(r), r))
    return slots


class Piece:
    def __init__(self, index, dims, order, src_of, dst_of):
        self.index, self.dims, self.order = index, dims, order
        self.src_of, self.dst_of = src_of, dst_of
        self.slots = piece_plan(dims, order)

    def locate(self, me, ranks):
        source, last, away = me, -1, None
        for place, (d, rank) in enumerate(zip(self.order, ranks)):
            if rank > 0:
                size, stride = self.dims[d]
                position = (me // stride) % size
                found, step = near(position, size, rank)
                source = source + (found - position) * stride
                last, away = place, step
        return source, last, away

    def sends(self, me, ranks):
        _, last, away = self.locate(me, ranks)
        out = []
        for place, d in enumerate(self.order):
            size, stride = self.dims[d]
            position = (me // stride) % size
            if place == last:
                if size > 2:
                    ok = jnp.logical_and(position + away >= 0, position + away < size)
                    out.append((ok, me + away * stride))
            elif place > last:
                if size == 2:
                    out.append((None, me + (1 - 2 * position) * stride))
                else:
                    out.append((position + 1 < size, me + stride))
                    out.append((position > 0, me - stride))
        return out


def when(condition, act):
    if condition is None:
        act()
    else:
        pl.when(condition)(act)


def spread(pieces, me, chunk, send_sem, recv_sem, low, high, mode):
    todo = []
    for piece in pieces:
        for ranks in piece.slots:
            todo.append((sum(ranks), piece, ranks))
    todo.sort(key=lambda t: t[0])
    for depth, piece, ranks in todo:
        if not low <= depth < high:
            continue
        source, last, _ = piece.locate(me, ranks)
        landed = piece.dst_of(chunk, source)
        origin = piece.src_of(chunk) if depth == 0 else landed
        recv = recv_sem.at[chunk, piece.index, source]
        if depth > 0 and mode == "start":
            pltpu.make_async_copy(landed, landed, recv).wait()
        base = piece.first_send[ranks]
        for offset, (ok, target) in enumerate(piece.sends(me, ranks)):
            copy = pltpu.make_async_remote_copy(
                src_ref=origin,
                dst_ref=landed,
                send_sem=send_sem.at[chunk, base + offset],
                recv_sem=recv,
                device_id={"fs": target},
                device_id_type=MESH,
            )
            when(ok, copy.start if mode == "start" else copy.wait_send)


def number_sends(pieces):
    total = 0
    for piece in pieces:
        piece.first_send = {}
        for ranks in piece.slots:
            piece.first_send[ranks] = total
            last = max([i for i, r in enumerate(ranks) if r > 0], default=-1)
            for place, d in enumerate(piece.order):
                size = piece.dims[d][0]
                if place == last:
                    total += 1 if size > 2 else 0
                elif place > last:
                    total += 1 if size == 2 else 2
    return total


def cut(extent, unit, share):
    return max(unit, min(extent - unit, round(extent * share / unit) * unit))


def gather_plan(dims, refs, outs, blocks):
    gate, up, down, mix_in, mix_out = refs
    gate_o, up_o, down_o, mix_in_o, mix_out_o = outs
    n = len(dims)
    first = tuple(range(n))
    second = first[1:] + first[:1]
    third = first[-1:] + first[:-1]
    pooled = mix_out.shape[0]

    def rows(ref, out, start_of, size):
        return (
            lambda c: ref.at[pl.ds(start_of(c), size), :],
            lambda c, s: out.at[s, pl.ds(start_of(c), size), :],
        )

    def at(block, offset):
        return lambda c: pl.multiple_of(c * block + offset, 16)

    block, tall = gate.shape[0] // blocks, down.shape[0] // blocks
    down_cut = cut(tall, 16, 2 / 3)
    main = [
        Piece(0, dims, first, *rows(gate, gate_o, at(block, 0), block)),
        Piece(1, dims, third, *rows(up, up_o, at(block, 0), block)),
        Piece(2, dims, first, *rows(down, down_o, at(tall, 0), down_cut)),
        Piece(3, dims, second, *rows(down, down_o, at(tall, down_cut), tall - down_cut)),
    ]
    mix_cut = cut(pooled, 16, 2 / 3)

    def fixed(offset):
        return lambda c: offset

    mix = [
        Piece(0, dims, first, *rows(mix_in, mix_in_o, fixed(0), mix_in.shape[0])),
        Piece(1, dims, third, *rows(mix_out, mix_out_o, fixed(0), mix_cut)),
        Piece(2, dims, second, *rows(mix_out, mix_out_o, fixed(mix_cut), pooled - mix_cut)),
    ]
    return main, mix


def gather_kernel(dims, blocks, *args):
    refs, outs = args[:5], args[5:10]
    beside = None
    if len(args) > 13:
        beside = args[10:12]
        args = args[:10] + args[12:]
    send_sem, recv_sem, local_sem = args[10:13]
    me = lax.axis_index("fs")
    barrier = pltpu.get_barrier_semaphore()
    expected = 0
    for size, stride in dims:
        position = (me // stride) % size
        for step, ok in ((1, position + 1 < size), (-1, position > 0)):
            def signal(step=step, stride=stride):
                pl.semaphore_signal(
                    barrier, inc=1, device_id={"fs": me + step * stride}, device_id_type=MESH
                )

            pl.when(ok)(signal)
            expected = expected + jnp.where(ok, 1, 0)
    pl.semaphore_wait(barrier, expected)

    main, mix = gather_plan(dims, refs, outs, blocks)
    number_sends(main)
    number_sends(mix)
    deepest = sum(size - 1 for size, _ in dims) + 1
    early = min(3, deepest)

    locals_ = []
    for i, (ref, out) in enumerate(zip(refs, outs)):
        if beside is not None and i in (2, 4):
            continue
        locals_.append(pltpu.make_async_copy(ref, out.at[me], local_sem.at[i]))

    go = functools.partial(spread, send_sem=send_sem, recv_sem=recv_sem)
    def shard_in(source, stage, sem, shard, across):
        return pltpu.make_async_copy(
            source, stage.at[:, pl.ds(shard * across, across)], sem.at[shard]
        )

    def lay_in(own, part, stage, sem, rows, height):
        for shard in range(part.shape[0]):
            for mine, source in ((True, own), (False, part.at[shard])):

                @pl.when((me == shard) if mine else (me != shard))
                def _(source=source, shard=shard):
                    piece = source.at[pl.ds(rows, height), :]
                    shard_in(piece, stage, sem, shard, part.shape[2]).start()

    def lay_out(part, whole, stage, sem, rows, height, mode):
        if mode == "start":
            for shard in range(part.shape[0]):
                piece = part.at[shard, pl.ds(rows, height), :]
                shard_in(piece, stage, sem, shard, part.shape[2]).wait()
        copy = pltpu.make_async_copy(
            stage, whole.at[pl.ds(rows, height), :], sem.at[part.shape[0]]
        )
        copy.start() if mode == "start" else copy.wait()

    if beside is not None:
        down_stage, mix_stage, down_sem, mix_sem = args[13:]
        tall = down_stage.shape[1]

        pooled = mix_stage.shape[0]

    def rows_of(c):
        return c * tall if isinstance(c, int) else pl.multiple_of(c * tall, 16)

    def down_in(c):
        slot = c % 2
        lay_in(refs[2], outs[2], down_stage.at[slot], down_sem.at[slot], rows_of(c), tall)

    def down_out(c, mode="start"):
        slot = c % 2
        lay_out(outs[2], beside[0], down_stage.at[slot], down_sem.at[slot], rows_of(c), tall, mode)

    go(mix, me, blocks, low=0, high=1, mode="start")
    go(main, me, 0, low=0, high=1, mode="start")
    for copy in locals_:
        copy.start()
    go(mix, me, blocks, low=1, high=deepest, mode="start")
    if beside is not None:
        lay_in(refs[4], outs[4], mix_stage, mix_sem, 0, pooled)

    def step(i, carry):
        @pl.when(i + 1 < blocks)
        def _():
            go(main, me, i + 1, low=0, high=1, mode="start")

        go(main, me, i, low=1, high=early, mode="start")

        @pl.when(i > 0)
        def _():
            go(main, me, i - 1, low=early, high=deepest, mode="start")

        if beside is not None:

            @pl.when(i > 2)
            def _():
                down_out(i - 3, "end")

            @pl.when(i > 0)
            def _():
                down_in(i - 1)

            @pl.when(i > 1)
            def _():
                down_out(i - 2)

        return carry

    lax.fori_loop(0, blocks, step, 0)
    go(main, me, blocks - 1, low=early, high=deepest, mode="start")
    if beside is not None:
        if blocks > 2:
            down_out(blocks - 3, "end")
        down_in(blocks - 1)
        if blocks > 1:
            down_out(blocks - 2)
        lay_out(outs[4], beside[1], mix_stage, mix_sem, 0, pooled, "start")
        down_out(blocks - 1)

    def finish(i, carry):
        go(main, me, i, low=0, high=deepest, mode="end")
        return carry

    lax.fori_loop(0, blocks, finish, 0)
    go(mix, me, blocks, low=0, high=deepest, mode="end")
    if beside is not None:
        if blocks > 1:
            down_out(blocks - 2, "end")
        down_out(blocks - 1, "end")
        lay_out(outs[4], beside[1], mix_stage, mix_sem, 0, pooled, "end")
    for copy in locals_:
        copy.wait()


def gather_weights(dims, w_gate, w_up, w_down, w_mix_in, w_mix_out):
    count = 1
    for size, _ in dims:
        count *= size
    tiles = (w_gate.shape[0] // 16, w_down.shape[0] // 16)
    blocks = next(b for b in (8, 4, 2, 1) if tiles[0] % b == 0 and tiles[1] % b == 0)
    weights = (w_gate, w_up, w_down, w_mix_in, w_mix_out)
    shapes = [jax.ShapeDtypeStruct((count, *a.shape), a.dtype) for a in weights]

    class Shape:
        def __init__(self, shape):
            self.shape = shape

    stand_in = [Shape(a.shape) for a in weights]
    main, mix = gather_plan(dims, stand_in, [Shape(s.shape) for s in shapes], blocks)
    sends = max(number_sends(main), number_sends(mix))
    scratch = [
        pltpu.SemaphoreType.DMA((blocks + 1, sends)),
        pltpu.SemaphoreType.DMA((blocks + 1, len(main), count)),
        pltpu.SemaphoreType.DMA((5,)),
    ]
    laid = w_down.shape[1] % 128 == 0
    if laid:
        tall, full = w_down.shape[0] // blocks, w_down.shape[1] * count
        shapes += [jax.ShapeDtypeStruct((a.shape[0], full), a.dtype) for a in (w_down, w_mix_out)]
        scratch += [
            pltpu.VMEM((2, tall, full), w_down.dtype),
            pltpu.VMEM((w_mix_out.shape[0], full), w_mix_out.dtype),
            pltpu.SemaphoreType.DMA((2, count + 1)),
            pltpu.SemaphoreType.DMA((count + 1,)),
        ]
    outs = pl.pallas_call(
        functools.partial(gather_kernel, dims, blocks),
        out_shape=shapes,
        in_specs=[pl.BlockSpec(memory_space=pltpu.HBM)] * 5,
        out_specs=[pl.BlockSpec(memory_space=pltpu.HBM)] * len(shapes),
        scratch_shapes=scratch,
        compiler_params=pltpu.CompilerParams(collective_id=0, has_side_effects=True),
        name="gather_weights",
    )(*weights)

    def stacked(a):
        return a.reshape(-1, a.shape[2])

    def beside(a):
        return jnp.transpose(a, (1, 0, 2)).reshape(a.shape[1], -1)

    gate, up, down, mix_in, mix_out = outs[:5]
    if laid:
        return stacked(gate), stacked(up), outs[5], stacked(mix_in), outs[6]
    return stacked(gate), stacked(up), beside(down), stacked(mix_in), beside(mix_out)


def rms_scale(values, gain):
    return values * lax.rsqrt(jnp.mean(values * values, axis=-1, keepdims=True) + 1e-06) * gain


def total_over_tp(left_rows, right_matrix):
    part = jnp.dot(left_rows, right_matrix, preferred_element_type=jnp.float32)
    part = part.astype(jnp.bfloat16)
    if lax.axis_size("tp") == 2:
        other = lax.ppermute(part, "tp", ((0, 1), (1, 0)))
        return part.astype(jnp.float32) + other.astype(jnp.float32)
    return lax.psum(part.astype(jnp.float32), "tp")


def own_total_over_tp(left_rows, right_matrix):
    part = jnp.dot(left_rows, right_matrix, preferred_element_type=jnp.float32)
    part = part.astype(jnp.bfloat16)
    if lax.axis_size("tp") == 2:
        mine = own_rows_of(part)
        half = mine.shape[0]
        theirs = lax.dynamic_slice_in_dim(part, (1 - lax.axis_index("tp")) * half, half, 0)
        other = lax.ppermute(theirs, "tp", ((0, 1), (1, 0)))
        return mine.astype(jnp.float32) + other.astype(jnp.float32)
    return lax.psum_scatter(part.astype(jnp.float32), "tp", scatter_dimension=0, tiled=True)


def own_rows_of(array):
    count = array.shape[0] // lax.axis_size("tp")
    return lax.dynamic_slice_in_dim(array, lax.axis_index("tp") * count, count, 0)


def body(dims, tokens, w_gate, w_up, w_down, w_mix_in, w_mix_out, pool_w, pool_scale, norm_gains):
    rows_all = tokens.shape[0]
    stream = tokens.astype(jnp.float32)
    normed = rms_scale(stream, norm_gains[0]).astype(jnp.bfloat16)
    gate_full, up_full, down_full, mix_in_full, mix_out_full = gather_weights(
        dims, w_gate, w_up, w_down, w_mix_in, w_mix_out
    )
    gate_first = jnp.dot(normed, gate_full, preferred_element_type=jnp.float32)
    up_first = jnp.dot(normed, up_full, preferred_element_type=jnp.float32)
    hidden = (jax.nn.silu(gate_first) * up_first).astype(jnp.bfloat16)
    stream = stream + 0.5 * rms_scale(total_over_tp(hidden, down_full), norm_gains[1])
    normed = rms_scale(stream, norm_gains[2]).astype(jnp.bfloat16)
    pooled_in = jnp.dot(normed, mix_in_full, preferred_element_type=jnp.float32)
    pooled_in = pooled_in.astype(jnp.bfloat16)
    groups_here = pool_w.shape[0]
    group_dim = pool_w.shape[1]
    values = pooled_in.astype(jnp.float32).reshape(rows_all // LEN, LEN, groups_here, group_dim)
    totals = jnp.cumsum(values, axis=1)
    position = jnp.arange(1, LEN + 1).astype(jnp.float32)[None, :, None, None]
    window_ids = (lax.axis_index("tp") * groups_here + jnp.arange(groups_here)) % 4
    average = jnp.zeros_like(values)
    for window_slot in range(4):
        window = 2 ** (1 + window_slot)
        lagged = jnp.pad(totals, ((0, 0), (window, 0), (0, 0), (0, 0)))[:, :LEN]
        candidate = (totals - lagged) / jnp.minimum(position, float(window))
        average = jnp.where((window_ids == window_slot)[None, None, :, None], candidate, average)
    deviation = (average - values).astype(jnp.bfloat16)
    regrouped = jnp.einsum("btgi,gio->btgo", deviation, pool_w, preferred_element_type=jnp.float32)
    regrouped = (
        regrouped.reshape(rows_all, groups_here * group_dim) * pool_scale.astype(jnp.float32)
    ).astype(jnp.bfloat16)
    stream = stream + rms_scale(total_over_tp(regrouped, mix_out_full), norm_gains[3])
    normed = rms_scale(stream, norm_gains[4]).astype(jnp.bfloat16)
    gate_second = jnp.dot(normed, gate_full, preferred_element_type=jnp.float32)
    up_second = jnp.dot(normed, up_full, preferred_element_type=jnp.float32)
    hidden = (jax.nn.silu(gate_second) * up_second).astype(jnp.bfloat16)
    stream_own = own_rows_of(stream)
    stream_own = stream_own + 0.5 * rms_scale(own_total_over_tp(hidden, down_full), norm_gains[5])
    return stream_own.astype(jnp.bfloat16)


def solution(mesh):
    in_specs = (
        P("fs", None),
        P("fs", "tp"),
        P("fs", "tp"),
        P("tp", "fs"),
        P("fs", "tp"),
        P("tp", "fs"),
        P("tp", None, None),
        P("tp"),
        P(),
    )
    out_specs = P(("fs", "tp"), None)
    return jax.shard_map(functools.partial(body, line_dims(mesh)), mesh=mesh, in_specs=in_specs, out_specs=out_specs, check_vma=False)
```
